32 devices in a mesh: sp: 8 (over z, y), tp: 4 (over x, core).
Axes of the slice: x: 2, y: 2, z: 4, core: 2. Of those that a mesh axis runs over, the one named last changes fastest.
Arguments:
- queries: bfloat16 [2048, 2048], P('sp', 'tp'), may hold values from -6 to 6
- keys: bfloat16 [2048, 512], P('sp', 'tp'), may hold values from -6 to 6
- values: bfloat16 [2048, 512], P('sp', 'tp'), may hold values from -6 to 6
- query_gain: float32 [64], replicated, may hold values from 0.8 to 5
- key_gain: float32 [64], replicated, may hold values from 0.8 to 5
- stream: bfloat16 [2048, 2048], P('sp'), may hold values from -0.1796875 to 0.1796875
- out_weight: bfloat16 [2048, 2048], P('tp'), may hold values from -0.125 to 0.125
- mixer_gain: float32 [2048], replicated, may hold values from 0.1 to 1.9
- up_weight: bfloat16 [2048, 8192], P('sp', 'tp'), may hold values from -0.125 to 0.125
- down_weight: bfloat16 [8192, 2048], P('tp', 'sp'), may hold values from -0.0625 to 0.0625
Outputs:
- updated: bfloat16 [2048, 2048], P('sp', 'tp')
The draws below stay inside these ranges and needn't reach their ends.
All inputs are finite; a program needn't handle non-finite values.
Results may differ from the reference program's by a relative error of at most 0.02.
The reference program's roundings to bfloat16 on the way count: a program that leaves them out, or rounds other values in their place, can miss the bound.
Values may be sent and summed in bfloat16 or wider, within the bound.
A program may use at most 128 MiB of HBM per device.

```python
import math
import jax
import jax.numpy as jnp
from jax import lax

D = 2048
HQ = 32
KVH = 8
HD = 64
FF = 8192
GRID_W = 64
TOKENS = 2048
N_TP = 4


def drawn(key):
    query_key = jax.random.fold_in(key, 101)
    key_key = jax.random.fold_in(key, 202)
    key_draw = jax.random.normal(key_key, (TOKENS, KVH * HD), jnp.float32)
    query_draw = jax.random.normal(query_key, (TOKENS, HQ * HD), jnp.float32)
    return (jnp.clip(query_draw, -6.0, 6.0), jnp.clip(key_draw, -6.0, 6.0))


def draw_queries(key, part):
    return drawn(key)[0].astype(jnp.bfloat16)


def draw_keys(key, part):
    return drawn(key)[1].astype(jnp.bfloat16)


def gain_draw(key, salt):
    gain_key = jax.random.fold_in(key, salt)
    return jax.random.uniform(gain_key, (HD,), jnp.float32, 0.8, 1.8)


def draw_query_gain(key, part):
    return gain_draw(key, 303)


def draw_key_gain(key, part):
    return gain_draw(key, 404)


def shard_levels(key, extent, pieces, low, high):
    gain, own = 1.0, jax.random.fold_in(key, 6)
    for dim, shards_of in pieces:
        heights = jnp.exp(jax.random.uniform(jax.random.fold_in(own, dim), (shards_of,), jnp.float32, low / len(pieces), high / len(pieces)))
        gain = gain * jnp.repeat(heights, extent[dim] // shards_of).reshape([-1 if axis == dim else 1 for axis in range(len(extent))])
    return gain


def bell_draw(stream_key, shape, spread, limit, cuts=(), held_as=jnp.bfloat16):
    loudness = shard_levels(stream_key, shape, cuts, -0.22, 0.18) if cuts else 1.0
    array = jax.random.normal(stream_key, shape, jnp.float32) * spread * loudness
    return jnp.minimum(jnp.maximum(array, -limit), limit).astype(held_as)


def setup_inputs(seed: int = 0) -> dict:
    seeds = jax.random.split(jax.random.key(seed), 11)
    queries = draw_queries(jax.random.fold_in(seeds[10], 71), 0)
    keys = draw_keys(jax.random.fold_in(seeds[10], 71), 0)
    values = bell_draw(seeds[2], (TOKENS, KVH * HD), 1.0, 6.0, ((0, 8), (1, 4)))
    query_gain = draw_query_gain(jax.random.fold_in(seeds[10], 71), 0)
    key_gain = draw_key_gain(jax.random.fold_in(seeds[10], 71), 0)
    stream = bell_draw(seeds[5], (TOKENS, D), 0.03, 0.1796875, ((0, 8),))
    out_weight = bell_draw(seeds[6], (HQ * HD, D), (HQ * HD) ** -0.5, 0.125, ((0, 4),))
    mixer_gain = jnp.clip(1.0 + 0.18 * jax.random.normal(seeds[7], (D,), jnp.float32), 0.1, 1.9)
    up_weight = bell_draw(seeds[8], (D, FF), D ** -0.5, 0.125, ((0, 8), (1, 4)))
    down_weight = bell_draw(seeds[9], (FF, D), FF ** -0.5, 0.0625, ((0, 4), (1, 8)))
    return dict(queries=queries, keys=keys, values=values, query_gain=query_gain, key_gain=key_gain, stream=stream, out_weight=out_weight, mixer_gain=mixer_gain, up_weight=up_weight, down_weight=down_weight)


EPSILON = 1e-06

def prepare(projected, gain_vec, offset):
    row_count = projected.shape[0]
    head_count = projected.shape[1] // HD
    widened = projected.astype(jnp.float32).reshape(row_count, head_count, HD)
    widened = widened * lax.rsqrt(lax.optimization_barrier(jnp.mean(widened * widened, axis=-1, keepdims=True)) + EPSILON) * gain_vec
    position = offset + jnp.arange(row_count, dtype=jnp.int32)
    grid_row = (position // GRID_W).astype(jnp.float32)
    grid_col = (position % GRID_W).astype(jnp.float32)
    half_dim = HD // 2
    inverse = 1.0 / jnp.power(10000.0, jnp.arange(0, half_dim, 2, dtype=jnp.float32) / half_dim)
    angle = jnp.concatenate([grid_row[:, None] * inverse, grid_col[:, None] * inverse], axis=-1)
    cosine = jnp.cos(angle)[:, None, :]
    sine_table = jnp.sin(angle)[:, None, :]
    paired = widened.reshape(row_count, head_count, half_dim, 2)
    former = paired[..., 0]
    latter = paired[..., 1]
    rotated = jnp.stack([former * cosine - latter * sine_table, former * sine_table + latter * cosine], axis=-1)
    return rotated.reshape(row_count, head_count, HD).astype(jnp.bfloat16)

def grouped_sum(left, right, groups):
    width = left.shape[1] // groups
    total = jnp.zeros((left.shape[0], right.shape[1]), jnp.float32)
    for group_index in range(groups):
        term = jnp.dot(left[:, group_index * width:(group_index + 1) * width], right[group_index * width:(group_index + 1) * width], preferred_element_type=jnp.float32).astype(jnp.bfloat16)
        term = lax.optimization_barrier(term)
        total = total + term.astype(jnp.float32)
    return total

def reference(queries, keys, values, query_gain, key_gain, stream, out_weight, mixer_gain, up_weight, down_weight):
    group_size = HQ // KVH
    prepared_queries = prepare(queries, query_gain, 0)
    prepared_keys = prepare(keys, key_gain, 0)
    key_wide = prepared_keys.astype(jnp.float32)
    value_wide = values.reshape(TOKENS, KVH, HD).astype(jnp.float32)
    block_rows = math.gcd(TOKENS, 128)
    blocks = prepared_queries.reshape(TOKENS // block_rows, block_rows, KVH, group_size, HD)
    score_scale = 1.0 / math.sqrt(HD)

    def attend_rows(query_block):
        scores = jnp.einsum('qhgd,khd->hgqk', query_block.astype(jnp.float32), key_wide) * score_scale
        peak = lax.optimization_barrier(jnp.max(scores, axis=-1, keepdims=True))
        exps = jnp.exp(scores - peak)
        totals = lax.optimization_barrier(jnp.sum(exps, axis=-1))
        rounded = exps.astype(jnp.bfloat16)
        mixed = jnp.einsum('hgqk,khd->hgqd', rounded.astype(jnp.float32), value_wide)
        mixed = mixed / totals[..., None]
        return jnp.transpose(mixed, (2, 0, 1, 3)).reshape(block_rows, HQ * HD).astype(jnp.bfloat16)
    head_out = lax.map(attend_rows, blocks).reshape(TOKENS, HQ * HD)
    attended = grouped_sum(head_out, out_weight, N_TP)
    mid = (stream.astype(jnp.float32) + attended).astype(jnp.bfloat16)
    mid_wide = mid.astype(jnp.float32)
    normed = mid_wide * lax.rsqrt(lax.optimization_barrier(jnp.mean(mid_wide * mid_wide, axis=-1, keepdims=True)) + EPSILON) * mixer_gain
    normed = normed.astype(jnp.bfloat16)
    up_sums = jnp.dot(normed, up_weight, preferred_element_type=jnp.float32)
    hidden = jnp.square(jax.nn.relu(up_sums)).astype(jnp.bfloat16)
    down_sums = grouped_sum(hidden, down_weight, N_TP)
    return (mid_wide + down_sums).astype(jnp.bfloat16)
```

```python
import functools
import math

import jax
import jax.numpy as jnp
from jax import lax
from jax.experimental import pallas as pl
from jax.experimental.pallas import tpu as pltpu
from jax.sharding import PartitionSpec as P

HD = 64
GRID_W = 64


EPSILON = 1e-06


def prepare(projected, gain_vec, offset):
    row_count = projected.shape[0]
    head_count = projected.shape[1] // HD
    widened = projected.astype(jnp.float32).reshape(row_count, head_count, HD)
    widened = (
        widened
        * lax.rsqrt(jnp.mean(widened * widened, axis=-1, keepdims=True) + EPSILON)
        * gain_vec
    )
    position = offset + jnp.arange(row_count, dtype=jnp.int32)
    grid_row = (position // GRID_W).astype(jnp.float32)
    grid_col = (position % GRID_W).astype(jnp.float32)
    half_dim = HD // 2
    inverse = 1.0 / jnp.power(10000.0, jnp.arange(0, half_dim, 2, dtype=jnp.float32) / half_dim)
    angle = jnp.concatenate([grid_row[:, None] * inverse, grid_col[:, None] * inverse], axis=-1)
    cosine = jnp.cos(angle)[:, None, :]
    sine_table = jnp.sin(angle)[:, None, :]
    paired = widened.reshape(row_count, head_count, half_dim, 2)
    former = paired[..., 0]
    latter = paired[..., 1]
    rotated = jnp.stack(
        [former * cosine - latter * sine_table, former * sine_table + latter * cosine], axis=-1
    )
    return rotated.reshape(row_count, head_count, HD).astype(jnp.bfloat16)


def attend_block(state, grouped, key_block, value_block):
    running, totals, weighted = state
    scores = jnp.einsum("qhgd,khd->hgqk", grouped, key_block, preferred_element_type=jnp.float32)
    scores = scores * (1.0 / math.sqrt(HD))
    newest = jnp.maximum(running, jnp.max(scores, axis=-1))
    rescale = jnp.exp(running - newest)
    exps = jnp.exp(scores - newest[..., None])
    totals = totals * rescale + jnp.sum(exps, axis=-1)
    weighted = weighted * rescale[..., None] + jnp.einsum(
        "hgqk,khd->hgqd", exps.astype(jnp.bfloat16), value_block, preferred_element_type=jnp.float32
    )
    return (newest, totals, weighted)


def shards(
    queries,
    keys,
    values,
    query_gain,
    key_gain,
    stream,
    out_weight,
    mixer_gain,
    up_weight,
    down_weight,
):
    local_rows = queries.shape[0]
    offset = lax.axis_index("sp") * local_rows
    kv_count = keys.shape[1] // HD
    group_size = queries.shape[1] // HD // kv_count
    grouped = prepare(queries, query_gain, offset).reshape(local_rows, kv_count, group_size, HD)
    prepared_keys = prepare(keys, key_gain, offset).reshape(local_rows, kv_count * HD)
    initial = (
        jnp.full((kv_count, group_size, local_rows), -1e30, jnp.float32),
        jnp.zeros((kv_count, group_size, local_rows), jnp.float32),
        jnp.zeros((kv_count, group_size, local_rows, HD), jnp.float32),
    )
    key_rows = lax.all_gather(prepared_keys, "sp", axis=0, tiled=True)
    value_rows = lax.all_gather(values, "sp", axis=0, tiled=True)
    piece_rows = key_rows.shape[0]
    block_rows = piece_rows if piece_rows <= 2048 else math.gcd(piece_rows, 2048)
    key_blocks = key_rows.reshape(piece_rows // block_rows, block_rows, kv_count, HD)
    value_blocks = value_rows.reshape(piece_rows // block_rows, block_rows, kv_count, HD)

    def visit_block(block_index, state_now):
        return attend_block(state_now, grouped, key_blocks[block_index], value_blocks[block_index])

    running, totals, weighted = lax.fori_loop(0, piece_rows // block_rows, visit_block, initial)
    head_out = weighted / totals[..., None]
    head_out = jnp.transpose(head_out, (2, 0, 1, 3)).reshape(local_rows, -1).astype(jnp.bfloat16)
    partial_value = jnp.dot(head_out, out_weight, preferred_element_type=jnp.float32)
    model_width = partial_value.shape[1]
    share_cols = model_width // lax.axis_size("tp")
    first_col = lax.axis_index("tp") * share_cols
    summed = lax.psum(partial_value.astype(jnp.bfloat16), "tp").astype(jnp.float32)
    mid = (stream.astype(jnp.float32) + summed).astype(jnp.bfloat16)
    mid_wide = mid.astype(jnp.float32)
    normed = (
        mid_wide
        * lax.rsqrt(jnp.mean(mid_wide * mid_wide, axis=-1, keepdims=True) + EPSILON)
        * mixer_gain
    )
    normed = normed.astype(jnp.bfloat16)
    own_mid = lax.dynamic_slice_in_dim(mid, first_col, share_cols, 1)
    up_sums = jnp.dot(
        normed,
        lax.all_gather(up_weight, "sp", axis=0, tiled=True),
        preferred_element_type=jnp.float32,
    )
    hidden = jnp.square(jax.nn.relu(up_sums)).astype(jnp.bfloat16)
    down_part = jnp.dot(
        hidden,
        lax.all_gather(down_weight, "sp", axis=1, tiled=True),
        preferred_element_type=jnp.float32,
    )
    down_share = lax.psum_scatter(
        down_part.astype(jnp.bfloat16), "tp", scatter_dimension=1, tiled=True
    ).astype(jnp.float32)
    return (own_mid.astype(jnp.float32) + down_share).astype(jnp.bfloat16)


def layer_kernel(
    planes,
    ranks,
    q_ref,
    kv_ref,
    stream_ref,
    out_w_ref,
    gain_ref,
    up_ref,
    down_ref,
    out_ref,
    kv_all,
    up_all,
    down_all,
    head_all,
    first_send,
    first_land,
    pair_send,
    pair_land,
    mid_all,
    core_send,
    core_land,
    core_keep,
    x_send,
    x_land,
    z_send,
    z_land,
    send_sems,
    recv_sems,
):
    rows = out_ref.shape[0]
    cols = out_ref.shape[1]
    lanes = q_ref.shape[2]
    slab = up_ref.shape[1] // planes
    depth = up_ref.shape[0]
    own_sp = lax.axis_index("sp")
    own_tp = lax.axis_index("tp")
    plane, side = own_sp // 2, own_sp % 2
    ex, core = own_tp // 2, own_tp % 2
    y_peer = (plane * 2 + 1 - side, own_tp)
    core_peer = (own_sp, ex * 2 + 1 - core)
    x_peer = (own_sp, (1 - ex) * 2 + core)

    def plane_at(offset):
        return lax.rem(plane + offset + planes, planes)

    def z_peer(offset):
        return (plane_at(offset) * 2 + side, own_tp)

    barrier = pltpu.get_barrier_semaphore()
    greeted = [y_peer, core_peer, x_peer] + [z_peer(d) for d in range(1, planes)]
    for peer in greeted:
        pl.semaphore_signal(barrier, inc=1, device_id=peer, device_id_type=pl.DeviceIdType.MESH)
    pl.semaphore_wait(barrier, len(greeted))

    copies = []

    def push(src, dst, peer):
        slot = len(copies)
        copy = pltpu.make_async_remote_copy(
            src_ref=src,
            dst_ref=dst,
            send_sem=send_sems.at[slot],
            recv_sem=recv_sems.at[slot],
            device_id=peer,
            device_id_type=pl.DeviceIdType.MESH,
        )
        copy.start()
        copies.append(copy)
        return copy

    def kv_at(sp):
        return kv_all.at[pl.ds(pl.multiple_of(sp * rows, rows), rows), :]

    def up_at(sp):
        return up_all.at[pl.ds(pl.multiple_of(sp * depth, depth), depth), :]

    def down_at(sp):
        return down_all.at[:, pl.ds(pl.multiple_of(sp * depth, depth), depth)]

    def up_part(p):
        return up_ref.at[:, pl.ds(pl.multiple_of(p * slab, slab), slab)]

    def down_part(p):
        return down_ref.at[pl.ds(pl.multiple_of(p * slab, slab), slab), :]

    kv_z = {d: push(kv_ref, kv_at(own_sp), z_peer(d)) for d in range(1, planes)}
    kv_y = {0: push(kv_ref, kv_at(own_sp), y_peer)}
    up_z, down_z = {}, {}
    for d in range(1, planes):
        up_z[d] = push(up_part(plane_at(d)), up_at(own_sp), z_peer(d))
        down_z[d] = push(down_part(plane_at(d)), down_at(own_sp), z_peer(d))
    kv_at(own_sp)[...] = kv_ref[...]
    up_at(own_sp)[...] = up_part(plane)[...]
    down_at(own_sp)[...] = down_part(plane)[...]
    for d in range(1, planes):
        kv_z[d].wait_recv()
        block = plane_at(-d) * 2 + side
        kv_y[d] = push(kv_at(block), kv_at(block), y_peer)
    up_y = {0: push(up_part(plane), up_at(own_sp), y_peer)}
    down_y = {0: push(down_part(plane), down_at(own_sp), y_peer)}
    for d in range(planes):
        kv_y[d].wait_recv()

    heads = q_ref.shape[0]
    kv_heads = lanes // HD
    pairs_each = heads // 2 // kv_heads

    def attend(h):
        scores = lax.dot_general(
            q_ref[h],
            kv_all[:, :lanes],
            (((1,), (1,)), ((), ())),
            preferred_element_type=jnp.float32,
        )
        exps = jnp.exp(scores - jnp.max(scores, axis=-1, keepdims=True))
        totals = jnp.sum(exps, axis=-1, keepdims=True)
        mixed = jnp.dot(
            exps.astype(jnp.bfloat16), kv_all[:, lanes:], preferred_element_type=jnp.float32
        )
        return mixed / totals

    def attend_pair(pair, carry):
        first, second = attend(2 * pair), attend(2 * pair + 1)
        low = pair < pairs_each
        left = jnp.where(low, first, pltpu.roll(first, HD, 1))
        right = jnp.where(low, pltpu.roll(second, HD, 1), second)
        lane = lax.broadcasted_iota(jnp.int32, left.shape, 1)
        head_all[pair] = jnp.where(lane < HD, left, right).astype(jnp.bfloat16)
        return carry

    lax.fori_loop(0, heads // 2, attend_pair, 0)

    def columns(rank):
        return pl.ds(pl.multiple_of(rank * cols, cols), cols)

    def project(rank):
        total = jnp.zeros((rows, cols), jnp.float32)
        for pair in range(heads // 2):
            total += jnp.dot(
                head_all[pair],
                out_w_ref[pair * lanes : (pair + 1) * lanes, columns(rank)],
                preferred_element_type=jnp.float32,
            )
        return total.astype(jnp.bfloat16)

    far, near = (1 - ex) * 2, ex * 2
    first_send[0] = project(far + 1 - core)
    pass_far = push(first_send.at[0], first_land.at[0], core_peer)
    first_send[1] = project(near + 1 - core)
    pass_near = push(first_send.at[1], first_land.at[1], core_peer)
    far_own = project(far + core).astype(jnp.float32)
    pass_far.wait_recv()
    pair_send[...] = (far_own + first_land[0].astype(jnp.float32)).astype(jnp.bfloat16)
    pass_x = push(pair_send, pair_land, x_peer)
    near_own = project(near + core).astype(jnp.float32)
    pass_near.wait_recv()
    near_own += first_land[1].astype(jnp.float32)
    near_own += stream_ref[:, columns(own_tp)].astype(jnp.float32)
    pass_x.wait_recv()
    mid = (near_own + pair_land[...].astype(jnp.float32)).astype(jnp.bfloat16)
    mid_all[plane, own_tp] = mid

    own_mid = mid_all.at[plane, own_tp]
    mid_z = {d: push(own_mid, own_mid, z_peer(d)) for d in range(1, planes)}
    mid_x = {0: push(own_mid, own_mid, x_peer)}
    mid_c = {0: push(own_mid, own_mid, core_peer)}
    mid_d = {}

    for d in range(1, planes):
        block = plane_at(-d) * 2 + side
        up_z[d].wait_recv()
        up_y[d] = push(up_at(block), up_at(block), y_peer)
        down_z[d].wait_recv()
        down_y[d] = push(down_at(block), down_at(block), y_peer)

    core_far, core_near, x_pass, z_pass = {}, {}, {}, {}

    def spread(d):
        mid_z[d].wait_recv()
        ref = mid_all.at[plane_at(-d), own_tp]
        mid_x[d] = push(ref, ref, x_peer)
        mid_c[d] = push(ref, ref, core_peer)

    def mix(d):
        where_z = plane_at(-d)
        wide = [mid_all[where_z, r].astype(jnp.float32) for r in range(ranks)]
        square = sum(jnp.sum(w * w, axis=-1, keepdims=True) for w in wide)
        inverse = lax.rsqrt(square / (ranks * cols) + EPSILON)
        sums = jnp.zeros((rows, slab), jnp.float32)
        for r in range(ranks):
            normed = wide[r] * inverse * gain_ref[:, r * cols : (r + 1) * cols]
            sums += jnp.dot(
                normed.astype(jnp.bfloat16),
                up_all[r * cols : (r + 1) * cols, :],
                preferred_element_type=jnp.float32,
            )
        return jnp.square(jnp.maximum(sums, 0.0)).astype(jnp.bfloat16)

    def lower(hidden, rank):
        part = jnp.dot(hidden, down_all[:, columns(rank)], preferred_element_type=jnp.float32)
        return part.astype(jnp.bfloat16)

    def core_stage(d):
        hidden = mix(d)
        core_send[d, 0] = lower(hidden, far + 1 - core)
        core_far[d] = push(core_send.at[d, 0], core_land.at[d, 0], core_peer)
        core_send[d, 1] = lower(hidden, near + 1 - core)
        core_near[d] = push(core_send.at[d, 1], core_land.at[d, 1], core_peer)
        core_keep[d, 0] = lower(hidden, far + core)
        core_keep[d, 1] = lower(hidden, near + core)

    def x_stage(d):
        core_far[d].wait_recv()
        x_send[d] = (
            core_keep[d, 0].astype(jnp.float32) + core_land[d, 0].astype(jnp.float32)
        ).astype(jnp.bfloat16)
        x_pass[d] = push(x_send.at[d], x_land.at[d], x_peer)

    def z_stage(d):
        core_near[d].wait_recv()
        x_pass[d].wait_recv()
        total = core_keep[d, 1].astype(jnp.float32) + core_land[d, 1].astype(jnp.float32)
        total += x_land[d].astype(jnp.float32)
        z_send[d] = total.astype(jnp.bfloat16)
        if d:
            z_pass[d] = push(z_send.at[d], z_land.at[d], z_peer(-d))

    for d in range(planes):
        if d + 1 < planes:
            spread(d + 1)
        mid_x[d].wait_recv()
        ref = mid_all.at[plane_at(-d), x_peer[1]]
        mid_d[d] = push(ref, ref, core_peer)
        if d == 0:
            for e in range(planes):
                up_y[e].wait_recv()
                down_y[e].wait_recv()
        mid_c[d].wait_recv()
        mid_d[d].wait_recv()
        core_stage(d)
        if d >= 1:
            x_stage(d - 1)
        if d >= 2:
            z_stage(d - 2)
    x_stage(planes - 1)
    for d in range(max(planes - 2, 0), planes):
        z_stage(d)
    total = mid_all[plane, own_tp].astype(jnp.float32) + z_send[0].astype(jnp.float32)
    for d in range(1, planes):
        z_pass[d].wait_recv()
        total += z_land[d].astype(jnp.float32)
    out_ref[...] = total.astype(jnp.bfloat16)
    for copy in copies:
        copy.wait_send()


def fused_shards(
    size_sp,
    size_tp,
    queries,
    keys,
    values,
    query_gain,
    key_gain,
    stream,
    out_weight,
    mixer_gain,
    up_weight,
    down_weight,
):
    planes = size_sp // 2
    rows, width = queries.shape
    lanes = keys.shape[1]
    heads = width // HD
    group_size = heads // (lanes // HD)
    cols = stream.shape[1] // size_tp
    offset = lax.axis_index("sp") * rows
    prepared_q = prepare(queries, query_gain, offset)
    prepared_k = prepare(keys, key_gain, offset).reshape(rows, lanes)
    prepared_q = jnp.transpose(prepared_q, (1, 0, 2)) * jnp.bfloat16(1.0 / math.sqrt(HD))
    blank = jnp.zeros_like(prepared_q[:group_size])
    padded = jnp.concatenate(
        [
            jnp.concatenate([prepared_q[:group_size], blank], axis=-1),
            jnp.concatenate([blank, prepared_q[group_size:]], axis=-1),
        ],
        axis=0,
    )
    kv = jnp.concatenate([prepared_k, values], axis=1)
    slab = up_weight.shape[1] // planes
    half = jnp.bfloat16
    tile = (rows, cols)
    total_copies = 64
    vmem = pl.BlockSpec(memory_space=pltpu.VMEM)
    scratch = [
        pltpu.VMEM((size_sp * rows, 2 * lanes), half),
        pltpu.VMEM((stream.shape[1], slab), half),
        pltpu.VMEM((slab, stream.shape[1]), half),
        pltpu.VMEM((heads // 2, rows, lanes), half),
        pltpu.VMEM((2,) + tile, half),
        pltpu.VMEM((2,) + tile, half),
        pltpu.VMEM(tile, half),
        pltpu.VMEM(tile, half),
        pltpu.VMEM((planes, size_tp) + tile, half),
        pltpu.VMEM((planes, 2) + tile, half),
        pltpu.VMEM((planes, 2) + tile, half),
        pltpu.VMEM((planes, 2) + tile, half),
        pltpu.VMEM((planes,) + tile, half),
        pltpu.VMEM((planes,) + tile, half),
        pltpu.VMEM((planes,) + tile, half),
        pltpu.VMEM((planes,) + tile, half),
        pltpu.SemaphoreType.DMA((total_copies,)),
        pltpu.SemaphoreType.DMA((total_copies,)),
    ]
    return pl.pallas_call(
        functools.partial(layer_kernel, planes, size_tp),
        out_shape=jax.ShapeDtypeStruct(tile, half),
        in_specs=[vmem] * 7,
        out_specs=vmem,
        scratch_shapes=scratch,
        compiler_params=pltpu.CompilerParams(
            collective_id=0, has_side_effects=True, vmem_limit_bytes=60 * 2**20
        ),
        name="layer",
    )(padded, kv, stream, out_weight, mixer_gain[None, :], up_weight, down_weight)


def solution(mesh):
    size_sp, size_tp = mesh.shape["sp"], mesh.shape["tp"]

    def body(*arrays):
        tiled = arrays[9].shape[1] % 128 == 0 and arrays[1].shape[1] == 2 * HD
        if tiled and size_tp == 4 and size_sp % 2 == 0:
            return fused_shards(size_sp, size_tp, *arrays)
        return shards(*arrays)

    return jax.shard_map(
        body,
        mesh=mesh,
        in_specs=(
            P("sp", "tp"),
            P("sp", "tp"),
            P("sp", "tp"),
            P(),
            P(),
            P("sp", None),
            P("tp", None),
            P(),
            P("sp", "tp"),
            P("tp", "sp"),
        ),
        out_specs=P("sp", "tp"),
        check_vma=False,
    )
```

```python
import functools
import math

import jax
import jax.numpy as jnp
from jax import lax
from jax.experimental import pallas as pl
from jax.experimental.pallas import tpu as pltpu
from jax.sharding import PartitionSpec as P

HD = 64
GRID_W = 64


EPSILON = 1e-06


def prepare(projected, gain_vec, offset):
    row_count = projected.shape[0]
    head_count = projected.shape[1] // HD
    widened = projected.astype(jnp.float32).reshape(row_count, head_count, HD)
    widened = (
        widened
        * lax.rsqrt(jnp.mean(widened * widened, axis=-1, keepdims=True) + EPSILON)
        * gain_vec
    )
    position = offset + jnp.arange(row_count, dtype=jnp.int32)
    grid_row = (position // GRID_W).astype(jnp.float32)
    grid_col = (position % GRID_W).astype(jnp.float32)
    half_dim = HD // 2
    inverse = 1.0 / jnp.power(10000.0, jnp.arange(0, half_dim, 2, dtype=jnp.float32) / half_dim)
    angle = jnp.concatenate([grid_row[:, None] * inverse, grid_col[:, None] * inverse], axis=-1)
    cosine = jnp.cos(angle)[:, None, :]
    sine_table = jnp.sin(angle)[:, None, :]
    paired = widened.reshape(row_count, head_count, half_dim, 2)
    former = paired[..., 0]
    latter = paired[..., 1]
    rotated = jnp.stack(
        [former * cosine - latter * sine_table, former * sine_table + latter * cosine], axis=-1
    )
    return rotated.reshape(row_count, head_count, HD).astype(jnp.bfloat16)


def attend_block(state, grouped, key_block, value_block):
    running, totals, weighted = state
    scores = jnp.einsum("qhgd,khd->hgqk", grouped, key_block, preferred_element_type=jnp.float32)
    scores = scores * (1.0 / math.sqrt(HD))
    newest = jnp.maximum(running, jnp.max(scores, axis=-1))
    rescale = jnp.exp(running - newest)
    exps = jnp.exp(scores - newest[..., None])
    totals = totals * rescale + jnp.sum(exps, axis=-1)
    weighted = weighted * rescale[..., None] + jnp.einsum(
        "hgqk,khd->hgqd", exps.astype(jnp.bfloat16), value_block, preferred_element_type=jnp.float32
    )
    return (newest, totals, weighted)


def shards(
    queries,
    keys,
    values,
    query_gain,
    key_gain,
    stream,
    out_weight,
    mixer_gain,
    up_weight,
    down_weight,
):
    local_rows = queries.shape[0]
    offset = lax.axis_index("sp") * local_rows
    kv_count = keys.shape[1] // HD
    group_size = queries.shape[1] // HD // kv_count
    grouped = prepare(queries, query_gain, offset).reshape(local_rows, kv_count, group_size, HD)
    prepared_keys = prepare(keys, key_gain, offset).reshape(local_rows, kv_count * HD)
    initial = (
        jnp.full((kv_count, group_size, local_rows), -1e30, jnp.float32),
        jnp.zeros((kv_count, group_size, local_rows), jnp.float32),
        jnp.zeros((kv_count, group_size, local_rows, HD), jnp.float32),
    )
    key_rows = lax.all_gather(prepared_keys, "sp", axis=0, tiled=True)
    value_rows = lax.all_gather(values, "sp", axis=0, tiled=True)
    piece_rows = key_rows.shape[0]
    block_rows = piece_rows if piece_rows <= 2048 else math.gcd(piece_rows, 2048)
    key_blocks = key_rows.reshape(piece_rows // block_rows, block_rows, kv_count, HD)
    value_blocks = value_rows.reshape(piece_rows // block_rows, block_rows, kv_count, HD)

    def visit_block(block_index, state_now):
        return attend_block(state_now, grouped, key_blocks[block_index], value_blocks[block_index])

    running, totals, weighted = lax.fori_loop(0, piece_rows // block_rows, visit_block, initial)
    head_out = weighted / totals[..., None]
    head_out = jnp.transpose(head_out, (2, 0, 1, 3)).reshape(local_rows, -1).astype(jnp.bfloat16)
    partial_value = jnp.dot(head_out, out_weight, preferred_element_type=jnp.float32)
    model_width = partial_value.shape[1]
    share_cols = model_width // lax.axis_size("tp")
    first_col = lax.axis_index("tp") * share_cols
    summed = lax.psum(partial_value.astype(jnp.bfloat16), "tp").astype(jnp.float32)
    mid = (stream.astype(jnp.float32) + summed).astype(jnp.bfloat16)
    mid_wide = mid.astype(jnp.float32)
    normed = (
        mid_wide
        * lax.rsqrt(jnp.mean(mid_wide * mid_wide, axis=-1, keepdims=True) + EPSILON)
        * mixer_gain
    )
    normed = normed.astype(jnp.bfloat16)
    own_mid = lax.dynamic_slice_in_dim(mid, first_col, share_cols, 1)
    up_sums = jnp.dot(
        normed,
        lax.all_gather(up_weight, "sp", axis=0, tiled=True),
        preferred_element_type=jnp.float32,
    )
    hidden = jnp.square(jax.nn.relu(up_sums)).astype(jnp.bfloat16)
    down_part = jnp.dot(
        hidden,
        lax.all_gather(down_weight, "sp", axis=1, tiled=True),
        preferred_element_type=jnp.float32,
    )
    down_share = lax.psum_scatter(
        down_part.astype(jnp.bfloat16), "tp", scatter_dimension=1, tiled=True
    ).astype(jnp.float32)
    return (own_mid.astype(jnp.float32) + down_share).astype(jnp.bfloat16)


def layer_kernel(
    planes,
    ranks,
    q_ref,
    k_ref,
    v_ref,
    tables_ref,
    gains_ref,
    stream_ref,
    out_w_ref,
    gain_ref,
    up_ref,
    down_ref,
    out_ref,
    q_all,
    kv_all,
    up_all,
    down_all,
    head_all,
    first_send,
    first_land,
    pair_send,
    pair_land,
    mid_all,
    core_send,
    core_land,
    core_keep,
    x_send,
    x_land,
    z_send,
    z_land,
    send_sems,
    recv_sems,
):
    rows = out_ref.shape[0]
    cols = out_ref.shape[1]
    lanes = q_all.shape[2]
    slab = up_ref.shape[1] // planes
    depth = up_ref.shape[0]
    own_sp = lax.axis_index("sp")
    own_tp = lax.axis_index("tp")
    plane, side = own_sp // 2, own_sp % 2
    ex, core = own_tp // 2, own_tp % 2
    y_peer = (plane * 2 + 1 - side, own_tp)
    core_peer = (own_sp, ex * 2 + 1 - core)
    x_peer = (own_sp, (1 - ex) * 2 + core)

    def plane_at(offset):
        return lax.rem(plane + offset + planes, planes)

    def z_peer(offset):
        return (plane_at(offset) * 2 + side, own_tp)

    def nearest(place):
        found = 0
        for p in range(planes):
            ranked = sorted(range(planes), key=lambda b: (abs(b - p), b if 2 * p < planes else -b))
            found = found + jnp.where(plane == p, ranked[place], 0)
        return found

    barrier = pltpu.get_barrier_semaphore()
    greeted = [y_peer, core_peer, x_peer] + [z_peer(d) for d in range(1, planes)]
    for peer in greeted:
        pl.semaphore_signal(barrier, inc=1, device_id=peer, device_id_type=pl.DeviceIdType.MESH)
    pl.semaphore_wait(barrier, len(greeted))

    copies = []

    slots = [0]

    def take(count):
        slots[0] += count
        return slots[0] - count

    def push(src, dst, peer):
        slot = take(1)
        copy = pltpu.make_async_remote_copy(
            src_ref=src,
            dst_ref=dst,
            send_sem=send_sems.at[slot],
            recv_sem=recv_sems.at[slot],
            device_id=peer,
            device_id_type=pl.DeviceIdType.MESH,
        )
        copy.start()
        copies.append(copy)
        return copy

    guarded = []

    def line(ref_of):
        base = take(planes + 2)

        def copy_of(b, send_slot, step):
            ref = ref_of(b)
            return pltpu.make_async_remote_copy(
                src_ref=ref,
                dst_ref=ref,
                send_sem=send_sems.at[send_slot],
                recv_sem=recv_sems.at[base + b],
                device_id=(jnp.clip(plane + step, 0, planes - 1) * 2 + side, own_tp),
                device_id_type=pl.DeviceIdType.MESH,
            )

        def begin(b, send_slot, step, valid):
            copy = copy_of(b, send_slot, step)
            pl.when(valid)(copy.start)
            guarded.append((valid, copy))

        def start(src=None):
            for slot, step, valid in (
                (planes, 1, plane < planes - 1),
                (planes + 1, -1, plane > 0),
            ):
                begin(plane, base + slot, step, valid)

        def arrive(b):
            copy_of(b, base + b, 1).wait_recv()
            begin(b, base + b, 1, jnp.logical_and(b < plane, plane < planes - 1))
            begin(b, base + b, -1, jnp.logical_and(b > plane, plane > 0))

        return start, arrive

    def kv_at(sp):
        return kv_all.at[pl.ds(pl.multiple_of(sp * rows, rows), rows), :]

    def up_at(sp):
        return up_all.at[pl.ds(pl.multiple_of(sp * depth, depth), depth), :]

    def down_at(sp):
        return down_all.at[:, pl.ds(pl.multiple_of(sp * depth, depth), depth)]

    def up_part(p):
        return up_ref.at[:, pl.ds(pl.multiple_of(p * slab, slab), slab)]

    def down_part(p):
        return down_ref.at[pl.ds(pl.multiple_of(p * slab, slab), slab), :]

    cosine, signed_sine = tables_ref[0], tables_ref[1]
    lane = lax.broadcasted_iota(jnp.int32, (rows, lanes), 1)
    is_low, is_even = lane < HD, lane % 2 == 0

    def turned(block, gain):
        wide = block.astype(jnp.float32)
        square = wide * wide
        low = jnp.sum(jnp.where(is_low, square, 0.0), axis=-1, keepdims=True)
        high = jnp.sum(jnp.where(is_low, 0.0, square), axis=-1, keepdims=True)
        wide = wide * lax.rsqrt(jnp.where(is_low, low, high) / HD + EPSILON) * gain
        partner = jnp.where(is_even, pltpu.roll(wide, lanes - 1, 1), pltpu.roll(wide, 1, 1))
        return (wide * cosine + partner * signed_sine).astype(jnp.bfloat16)

    own_rows = pl.ds(pl.multiple_of(own_sp * rows, rows), rows)
    kv_all[own_rows, :lanes] = turned(k_ref[...], gains_ref[1:2])
    kv_all[own_rows, lanes:] = v_ref[...]
    kv_start, kv_arrive = line(lambda b: kv_at(b * 2 + side))
    kv_start()
    kv_y = {0: push(kv_at(own_sp), kv_at(own_sp), y_peer)}
    up_z, down_z = {}, {}
    offsets = sorted(range(1, planes), key=lambda d: (d != planes // 2, d))
    for d in offsets:
        up_z[d] = push(up_part(plane_at(d)), up_at(own_sp), z_peer(d))
    for d in offsets:
        down_z[d] = push(down_part(plane_at(d)), down_at(own_sp), z_peer(d))
    up_at(own_sp)[...] = up_part(plane)[...]
    down_at(own_sp)[...] = down_part(plane)[...]
    blocks = q_ref.shape[1] // lanes
    for i in range(blocks):
        block = turned(q_ref[:, i * lanes : (i + 1) * lanes], gains_ref[0:1]).astype(jnp.float32)
        block = block * (1.0 / math.sqrt(HD))
        swapped = pltpu.roll(block, HD, 1)
        low = 2 * i < blocks
        mine = is_low if low else jnp.logical_not(is_low)
        pair = (block, swapped) if low else (swapped, block)
        for h in range(2):
            q_all[2 * i + h] = jnp.where(mine, pair[h], 0.0).astype(jnp.bfloat16)
    for d in range(1, planes):
        b = nearest(d)
        kv_arrive(b)
        kv_y[d] = push(kv_at(b * 2 + side), kv_at(b * 2 + side), y_peer)
    up_y = {0: push(up_part(plane), up_at(own_sp), y_peer)}
    down_y = {0: push(down_part(plane), down_at(own_sp), y_peer)}
    for d in range(planes):
        kv_y[d].wait_recv()

    def forward_up(d):
        block = plane_at(-d) * 2 + side
        up_z[d].wait_recv()
        up_y[d] = push(up_at(block), up_at(block), y_peer)

    def forward_down(d):
        block = plane_at(-d) * 2 + side
        down_z[d].wait_recv()
        down_y[d] = push(down_at(block), down_at(block), y_peer)

    heads = q_all.shape[0]
    kv_heads = lanes // HD
    pairs_each = heads // 2 // kv_heads

    def attend(h):
        scores = lax.dot_general(
            q_all[h],
            kv_all[:, :lanes],
            (((1,), (1,)), ((), ())),
            preferred_element_type=jnp.float32,
        )
        exps = jnp.exp(scores - jnp.max(scores, axis=-1, keepdims=True))
        totals = jnp.sum(exps, axis=-1, keepdims=True)
        mixed = jnp.dot(
            exps.astype(jnp.bfloat16), kv_all[:, lanes:], preferred_element_type=jnp.float32
        )
        return mixed / totals

    def attend_pair(pair, carry):
        first, second = attend(2 * pair), attend(2 * pair + 1)
        low = pair < pairs_each
        left = jnp.where(low, first, pltpu.roll(first, HD, 1))
        right = jnp.where(low, pltpu.roll(second, HD, 1), second)
        lane = lax.broadcasted_iota(jnp.int32, left.shape, 1)
        head_all[pair] = jnp.where(lane < HD, left, right).astype(jnp.bfloat16)
        return carry

    lax.fori_loop(0, heads // 2, attend_pair, 0)
    forward_up(offsets[0])

    def columns(rank):
        return pl.ds(pl.multiple_of(rank * cols, cols), cols)

    def project(rank):
        total = jnp.zeros((rows, cols), jnp.float32)
        for pair in range(heads // 2):
            total += jnp.dot(
                head_all[pair],
                out_w_ref[pair * lanes : (pair + 1) * lanes, columns(rank)],
                preferred_element_type=jnp.float32,
            )
        return total.astype(jnp.bfloat16)

    far, near = (1 - ex) * 2, ex * 2
    first_send[0] = project(far + 1 - core)
    pass_far = push(first_send.at[0], first_land.at[0], core_peer)
    first_send[1] = project(near + 1 - core)
    pass_near = push(first_send.at[1], first_land.at[1], core_peer)
    far_own = project(far + core).astype(jnp.float32)
    pass_far.wait_recv()
    pair_send[...] = (far_own + first_land[0].astype(jnp.float32)).astype(jnp.bfloat16)
    pass_x = push(pair_send, pair_land, x_peer)
    near_own = project(near + core).astype(jnp.float32)
    pass_near.wait_recv()
    near_own += first_land[1].astype(jnp.float32)
    near_own += stream_ref[:, columns(own_tp)].astype(jnp.float32)
    pass_x.wait_recv()
    mid = (near_own + pair_land[...].astype(jnp.float32)).astype(jnp.bfloat16)
    mid_all[plane, own_tp] = mid

    own_mid = mid_all.at[plane, own_tp]
    mid_start, mid_arrive = line(lambda b: mid_all.at[b, own_tp])
    mid_start()
    mid_x = {0: push(own_mid, own_mid, x_peer)}
    mid_c = {0: push(own_mid, own_mid, core_peer)}
    mid_d = {}
    for d in offsets[1:]:
        forward_up(d)
    for d in offsets:
        forward_down(d)

    core_far, core_near, x_pass, z_pass = {}, {}, {}, {}

    def spread(d):
        mid_arrive(nearest(d))
        ref = mid_all.at[nearest(d), own_tp]
        mid_x[d] = push(ref, ref, x_peer)
        mid_c[d] = push(ref, ref, core_peer)

    z_base = take(planes)

    def z_copy(d, target, sender):
        return pltpu.make_async_remote_copy(
            src_ref=z_send.at[d],
            dst_ref=z_land.at[sender],
            send_sem=send_sems.at[z_base + d],
            recv_sem=recv_sems.at[z_base + sender],
            device_id=(target * 2 + side, own_tp),
            device_id_type=pl.DeviceIdType.MESH,
        )

    def mix(d):
        where_z = nearest(d)
        wide = [mid_all[where_z, r].astype(jnp.float32) for r in range(ranks)]
        square = sum(jnp.sum(w * w, axis=-1, keepdims=True) for w in wide)
        inverse = lax.rsqrt(square / (ranks * cols) + EPSILON)
        sums = jnp.zeros((rows, slab), jnp.float32)
        for r in range(ranks):
            normed = wide[r] * inverse * gain_ref[:, r * cols : (r + 1) * cols]
            sums += jnp.dot(
                normed.astype(jnp.bfloat16),
                up_all[r * cols : (r + 1) * cols, :],
                preferred_element_type=jnp.float32,
            )
        return jnp.square(jnp.maximum(sums, 0.0)).astype(jnp.bfloat16)

    def lower(hidden, rank):
        part = jnp.dot(hidden, down_all[:, columns(rank)], preferred_element_type=jnp.float32)
        return part.astype(jnp.bfloat16)

    def core_stage(d):
        hidden = mix(d)
        core_send[d, 0] = lower(hidden, far + 1 - core)
        core_far[d] = push(core_send.at[d, 0], core_land.at[d, 0], core_peer)
        core_send[d, 1] = lower(hidden, near + 1 - core)
        core_near[d] = push(core_send.at[d, 1], core_land.at[d, 1], core_peer)
        core_keep[d, 0] = lower(hidden, far + core)
        core_keep[d, 1] = lower(hidden, near + core)

    def x_stage(d):
        core_far[d].wait_recv()
        x_send[d] = (
            core_keep[d, 0].astype(jnp.float32) + core_land[d, 0].astype(jnp.float32)
        ).astype(jnp.bfloat16)
        x_pass[d] = push(x_send.at[d], x_land.at[d], x_peer)

    def z_stage(d):
        core_near[d].wait_recv()
        x_pass[d].wait_recv()
        total = core_keep[d, 1].astype(jnp.float32) + core_land[d, 1].astype(jnp.float32)
        total += x_land[d].astype(jnp.float32)
        z_send[d] = total.astype(jnp.bfloat16)
        if d:
            z_pass[d] = z_copy(d, nearest(d), plane)
            z_pass[d].start()
            copies.append(z_pass[d])

    for d in range(planes):
        if d + 1 < planes:
            spread(d + 1)
        mid_x[d].wait_recv()
        ref = mid_all.at[nearest(d), x_peer[1]]
        mid_d[d] = push(ref, ref, core_peer)
        if d == 0:
            for e in range(planes):
                up_y[e].wait_recv()
                down_y[e].wait_recv()
        mid_c[d].wait_recv()
        mid_d[d].wait_recv()
        core_stage(d)
        if d >= 1:
            x_stage(d - 1)
        if d >= 2:
            z_stage(d - 2)
    x_stage(planes - 1)
    for d in range(max(planes - 2, 0), planes):
        z_stage(d)
    total = mid_all[plane, own_tp].astype(jnp.float32) + z_send[0].astype(jnp.float32)
    for d in range(1, planes):
        sender = nearest(d)
        z_copy(d, sender, sender).wait_recv()
        total += z_land[sender].astype(jnp.float32)
    out_ref[...] = total.astype(jnp.bfloat16)
    for copy in copies:
        copy.wait_send()
    for valid, copy in guarded:
        pl.when(valid)(copy.wait_send)


def fused_shards(
    size_sp,
    size_tp,
    queries,
    keys,
    values,
    query_gain,
    key_gain,
    stream,
    out_weight,
    mixer_gain,
    up_weight,
    down_weight,
):
    planes = size_sp // 2
    rows, width = queries.shape
    lanes = keys.shape[1]
    heads = width // HD
    cols = stream.shape[1] // size_tp
    position = lax.axis_index("sp") * rows + jnp.arange(rows, dtype=jnp.int32)
    grid_row = (position // GRID_W).astype(jnp.float32)[:, None]
    grid_col = (position % GRID_W).astype(jnp.float32)[:, None]
    lane = jnp.arange(lanes, dtype=jnp.int32)
    pair = lane % HD // 2
    quarter = HD // 4
    inverse = 1.0 / jnp.power(10000.0, (pair % quarter * 2).astype(jnp.float32) / (HD // 2))
    angle = jnp.where(pair < quarter, grid_row, grid_col) * inverse
    sine = jnp.sin(angle)
    tables = jnp.stack([jnp.cos(angle), jnp.where(lane % 2 == 0, -sine, sine)])
    gains = jnp.stack([jnp.tile(query_gain, lanes // HD), jnp.tile(key_gain, lanes // HD)])
    slab = up_weight.shape[1] // planes
    half = jnp.bfloat16
    tile = (rows, cols)
    total_copies = 96
    vmem = pl.BlockSpec(memory_space=pltpu.VMEM)
    scratch = [
        pltpu.VMEM((heads, rows, lanes), half),
        pltpu.VMEM((size_sp * rows, 2 * lanes), half),
        pltpu.VMEM((stream.shape[1], slab), half),
        pltpu.VMEM((slab, stream.shape[1]), half),
        pltpu.VMEM((heads // 2, rows, lanes), half),
        pltpu.VMEM((2,) + tile, half),
        pltpu.VMEM((2,) + tile, half),
        pltpu.VMEM(tile, half),
        pltpu.VMEM(tile, half),
        pltpu.VMEM((planes, size_tp) + tile, half),
        pltpu.VMEM((planes, 2) + tile, half),
        pltpu.VMEM((planes, 2) + tile, half),
        pltpu.VMEM((planes, 2) + tile, half),
        pltpu.VMEM((planes,) + tile, half),
        pltpu.VMEM((planes,) + tile, half),
        pltpu.VMEM((planes,) + tile, half),
        pltpu.VMEM((planes,) + tile, half),
        pltpu.SemaphoreType.DMA((total_copies,)),
        pltpu.SemaphoreType.DMA((total_copies,)),
    ]
    return pl.pallas_call(
        functools.partial(layer_kernel, planes, size_tp),
        out_shape=jax.ShapeDtypeStruct(tile, half),
        in_specs=[vmem] * 10,
        out_specs=vmem,
        scratch_shapes=scratch,
        compiler_params=pltpu.CompilerParams(
            collective_id=0, has_side_effects=True, vmem_limit_bytes=60 * 2**20
        ),
        name="layer",
    )(queries, keys, values, tables, gains, stream, out_weight, mixer_gain[None, :], up_weight, down_weight)


def solution(mesh):
    size_sp, size_tp = mesh.shape["sp"], mesh.shape["tp"]

    def body(*arrays):
        tiled = arrays[9].shape[1] % 128 == 0 and arrays[1].shape[1] == 2 * HD
        if tiled and size_tp == 4 and size_sp % 2 == 0:
            return fused_shards(size_sp, size_tp, *arrays)
        return shards(*arrays)

    return jax.shard_map(
        body,
        mesh=mesh,
        in_specs=(
            P("sp", "tp"),
            P("sp", "tp"),
            P("sp", "tp"),
            P(),
            P(),
            P("sp", None),
            P("tp", None),
            P(),
            P("sp", "tp"),
            P("tp", "sp"),
        ),
        out_specs=P("sp", "tp"),
        check_vma=False,
    )
```

```python
import functools
import math

import jax
import jax.numpy as jnp
from jax import lax
from jax.experimental import pallas as pl
from jax.experimental.pallas import tpu as pltpu
from jax.sharding import PartitionSpec as P

HD = 64
GRID_W = 64


EPSILON = 1e-06


def prepare(projected, gain_vec, offset):
    row_count = projected.shape[0]
    head_count = projected.shape[1] // HD
    widened = projected.astype(jnp.float32).reshape(row_count, head_count, HD)
    widened = (
        widened
        * lax.rsqrt(jnp.mean(widened * widened, axis=-1, keepdims=True) + EPSILON)
        * gain_vec
    )
    position = offset + jnp.arange(row_count, dtype=jnp.int32)
    grid_row = (position // GRID_W).astype(jnp.float32)
    grid_col = (position % GRID_W).astype(jnp.float32)
    half_dim = HD // 2
    inverse = 1.0 / jnp.power(10000.0, jnp.arange(0, half_dim, 2, dtype=jnp.float32) / half_dim)
    angle = jnp.concatenate([grid_row[:, None] * inverse, grid_col[:, None] * inverse], axis=-1)
    cosine = jnp.cos(angle)[:, None, :]
    sine_table = jnp.sin(angle)[:, None, :]
    paired = widened.reshape(row_count, head_count, half_dim, 2)
    former = paired[..., 0]
    latter = paired[..., 1]
    rotated = jnp.stack(
        [former * cosine - latter * sine_table, former * sine_table + latter * cosine], axis=-1
    )
    return rotated.reshape(row_count, head_count, HD).astype(jnp.bfloat16)


def attend_block(state, grouped, key_block, value_block):
    running, totals, weighted = state
    scores = jnp.einsum("qhgd,khd->hgqk", grouped, key_block, preferred_element_type=jnp.float32)
    scores = scores * (1.0 / math.sqrt(HD))
    newest = jnp.maximum(running, jnp.max(scores, axis=-1))
    rescale = jnp.exp(running - newest)
    exps = jnp.exp(scores - newest[..., None])
    totals = totals * rescale + jnp.sum(exps, axis=-1)
    weighted = weighted * rescale[..., None] + jnp.einsum(
        "hgqk,khd->hgqd", exps.astype(jnp.bfloat16), value_block, preferred_element_type=jnp.float32
    )
    return (newest, totals, weighted)


def shards(
    queries,
    keys,
    values,
    query_gain,
    key_gain,
    stream,
    out_weight,
    mixer_gain,
    up_weight,
    down_weight,
):
    local_rows = queries.shape[0]
    offset = lax.axis_index("sp") * local_rows
    kv_count = keys.shape[1] // HD
    group_size = queries.shape[1] // HD // kv_count
    grouped = prepare(queries, query_gain, offset).reshape(local_rows, kv_count, group_size, HD)
    prepared_keys = prepare(keys, key_gain, offset).reshape(local_rows, kv_count * HD)
    initial = (
        jnp.full((kv_count, group_size, local_rows), -1e30, jnp.float32),
        jnp.zeros((kv_count, group_size, local_rows), jnp.float32),
        jnp.zeros((kv_count, group_size, local_rows, HD), jnp.float32),
    )
    key_rows = lax.all_gather(prepared_keys, "sp", axis=0, tiled=True)
    value_rows = lax.all_gather(values, "sp", axis=0, tiled=True)
    piece_rows = key_rows.shape[0]
    block_rows = piece_rows if piece_rows <= 2048 else math.gcd(piece_rows, 2048)
    key_blocks = key_rows.reshape(piece_rows // block_rows, block_rows, kv_count, HD)
    value_blocks = value_rows.reshape(piece_rows // block_rows, block_rows, kv_count, HD)

    def visit_block(block_index, state_now):
        return attend_block(state_now, grouped, key_blocks[block_index], value_blocks[block_index])

    running, totals, weighted = lax.fori_loop(0, piece_rows // block_rows, visit_block, initial)
    head_out = weighted / totals[..., None]
    head_out = jnp.transpose(head_out, (2, 0, 1, 3)).reshape(local_rows, -1).astype(jnp.bfloat16)
    partial_value = jnp.dot(head_out, out_weight, preferred_element_type=jnp.float32)
    model_width = partial_value.shape[1]
    share_cols = model_width // lax.axis_size("tp")
    first_col = lax.axis_index("tp") * share_cols
    summed = lax.psum(partial_value.astype(jnp.bfloat16), "tp").astype(jnp.float32)
    mid = (stream.astype(jnp.float32) + summed).astype(jnp.bfloat16)
    mid_wide = mid.astype(jnp.float32)
    normed = (
        mid_wide
        * lax.rsqrt(jnp.mean(mid_wide * mid_wide, axis=-1, keepdims=True) + EPSILON)
        * mixer_gain
    )
    normed = normed.astype(jnp.bfloat16)
    own_mid = lax.dynamic_slice_in_dim(mid, first_col, share_cols, 1)
    up_sums = jnp.dot(
        normed,
        lax.all_gather(up_weight, "sp", axis=0, tiled=True),
        preferred_element_type=jnp.float32,
    )
    hidden = jnp.square(jax.nn.relu(up_sums)).astype(jnp.bfloat16)
    down_part = jnp.dot(
        hidden,
        lax.all_gather(down_weight, "sp", axis=1, tiled=True),
        preferred_element_type=jnp.float32,
    )
    down_share = lax.psum_scatter(
        down_part.astype(jnp.bfloat16), "tp", scatter_dimension=1, tiled=True
    ).astype(jnp.float32)
    return (own_mid.astype(jnp.float32) + down_share).astype(jnp.bfloat16)


def layer_kernel(
    planes,
    ranks,
    q_ref,
    k_ref,
    v_ref,
    tables_ref,
    gains_ref,
    stream_ref,
    out_w_ref,
    gain_ref,
    up_ref,
    down_ref,
    out_ref,
    q_all,
    kv_all,
    up_all,
    down_all,
    head_all,
    first_send,
    first_land,
    pair_send,
    pair_land,
    mid_all,
    core_send,
    core_land,
    core_keep,
    x_send,
    x_land,
    z_send,
    z_land,
    send_sems,
    recv_sems,
):
    rows = out_ref.shape[0]
    cols = out_ref.shape[1]
    lanes = q_all.shape[2]
    slab = up_ref.shape[1] // planes
    depth = up_ref.shape[0]
    own_sp = lax.axis_index("sp")
    own_tp = lax.axis_index("tp")
    plane, side = own_sp // 2, own_sp % 2
    ex, core = own_tp // 2, own_tp % 2
    y_peer = (plane * 2 + 1 - side, own_tp)
    core_peer = (own_sp, ex * 2 + 1 - core)
    x_peer = (own_sp, (1 - ex) * 2 + core)

    def plane_at(offset):
        return lax.rem(plane + offset + planes, planes)

    def z_peer(offset):
        return (plane_at(offset) * 2 + side, own_tp)

    def nearest(place):
        found = 0
        for p in range(planes):
            ranked = sorted(range(planes), key=lambda b: (abs(b - p), b if 2 * p < planes else -b))
            found = found + jnp.where(plane == p, ranked[place], 0)
        return found

    barrier = pltpu.get_barrier_semaphore()
    greeted = [y_peer, core_peer, x_peer] + [z_peer(d) for d in range(1, planes)]
    for peer in greeted:
        pl.semaphore_signal(barrier, inc=1, device_id=peer, device_id_type=pl.DeviceIdType.MESH)
    pl.semaphore_wait(barrier, len(greeted))

    copies = []

    slots = [0]

    def take(count):
        slots[0] += count
        return slots[0] - count

    def push(src, dst, peer):
        slot = take(1)
        copy = pltpu.make_async_remote_copy(
            src_ref=src,
            dst_ref=dst,
            send_sem=send_sems.at[slot],
            recv_sem=recv_sems.at[slot],
            device_id=peer,
            device_id_type=pl.DeviceIdType.MESH,
        )
        copy.start()
        copies.append(copy)
        return copy

    guarded = []

    def line(ref_of, relay):
        base = take(planes + 2)

        def straight():
            ref = ref_of(plane)
            for place in range(1, planes):
                copy = pltpu.make_async_remote_copy(
                    src_ref=ref,
                    dst_ref=ref,
                    send_sem=send_sems.at[base + place],
                    recv_sem=recv_sems.at[base + plane],
                    device_id=(nearest(place) * 2 + side, own_tp),
                    device_id_type=pl.DeviceIdType.MESH,
                )
                copy.start()
                copies.append(copy)

        def copy_of(b, send_slot, step):
            ref = ref_of(b)
            return pltpu.make_async_remote_copy(
                src_ref=ref,
                dst_ref=ref,
                send_sem=send_sems.at[send_slot],
                recv_sem=recv_sems.at[base + b],
                device_id=(jnp.clip(plane + step, 0, planes - 1) * 2 + side, own_tp),
                device_id_type=pl.DeviceIdType.MESH,
            )

        def begin(b, send_slot, step, valid):
            copy = copy_of(b, send_slot, step)
            pl.when(valid)(copy.start)
            guarded.append((valid, copy))

        def start():
            if not relay:
                return straight()
            for slot, step, valid in (
                (planes, 1, plane < planes - 1),
                (planes + 1, -1, plane > 0),
            ):
                begin(plane, base + slot, step, valid)

        def arrive(b):
            copy_of(b, base + b, 1).wait_recv()
            if not relay:
                return
            begin(b, base + b, 1, jnp.logical_and(b < plane, plane < planes - 1))
            begin(b, base + b, -1, jnp.logical_and(b > plane, plane > 0))

        return start, arrive

    def kv_at(sp):
        return kv_all.at[pl.ds(pl.multiple_of(sp * rows, rows), rows), :]

    def up_at(sp):
        return up_all.at[pl.ds(pl.multiple_of(sp * depth, depth), depth), :]

    def down_at(sp):
        return down_all.at[:, pl.ds(pl.multiple_of(sp * depth, depth), depth)]

    def up_part(p):
        return up_ref.at[:, pl.ds(pl.multiple_of(p * slab, slab), slab)]

    def down_part(p):
        return down_ref.at[pl.ds(pl.multiple_of(p * slab, slab), slab), :]

    cosine, signed_sine = tables_ref[0], tables_ref[1]
    lane = lax.broadcasted_iota(jnp.int32, (rows, lanes), 1)
    is_low, is_even = lane < HD, lane % 2 == 0

    def turned(block, gain):
        wide = block.astype(jnp.float32)
        square = wide * wide
        low = jnp.sum(jnp.where(is_low, square, 0.0), axis=-1, keepdims=True)
        high = jnp.sum(jnp.where(is_low, 0.0, square), axis=-1, keepdims=True)
        wide = wide * lax.rsqrt(jnp.where(is_low, low, high) / HD + EPSILON) * gain
        partner = jnp.where(is_even, pltpu.roll(wide, lanes - 1, 1), pltpu.roll(wide, 1, 1))
        return (wide * cosine + partner * signed_sine).astype(jnp.bfloat16)

    own_rows = pl.ds(pl.multiple_of(own_sp * rows, rows), rows)
    kv_all[own_rows, :lanes] = turned(k_ref[...], gains_ref[1:2])
    kv_all[own_rows, lanes:] = v_ref[...]
    kv_start, kv_arrive = line(lambda b: kv_at(b * 2 + side), False)
    kv_start()
    kv_y = {0: push(kv_at(own_sp), kv_at(own_sp), y_peer)}
    up_z, down_z = {}, {}
    offsets = sorted(range(1, planes), key=lambda d: (d != planes // 2, d))
    for d in offsets:
        up_z[d] = push(up_part(plane_at(d)), up_at(own_sp), z_peer(d))
    for d in offsets:
        down_z[d] = push(down_part(plane_at(d)), down_at(own_sp), z_peer(d))
    up_at(own_sp)[...] = up_part(plane)[...]
    down_at(own_sp)[...] = down_part(plane)[...]
    blocks = q_ref.shape[1] // lanes
    for i in range(blocks):
        block = turned(q_ref[:, i * lanes : (i + 1) * lanes], gains_ref[0:1]).astype(jnp.float32)
        block = block * (1.0 / math.sqrt(HD))
        swapped = pltpu.roll(block, HD, 1)
        low = 2 * i < blocks
        mine = is_low if low else jnp.logical_not(is_low)
        pair = (block, swapped) if low else (swapped, block)
        for h in range(2):
            q_all[2 * i + h] = jnp.where(mine, pair[h], 0.0).astype(jnp.bfloat16)
    for d in range(1, planes):
        b = nearest(d)
        kv_arrive(b)
        kv_y[d] = push(kv_at(b * 2 + side), kv_at(b * 2 + side), y_peer)
    up_y = {0: push(up_part(plane), up_at(own_sp), y_peer)}
    down_y = {0: push(down_part(plane), down_at(own_sp), y_peer)}
    for d in range(planes):
        kv_y[d].wait_recv()

    def forward_up(d):
        block = plane_at(-d) * 2 + side
        up_z[d].wait_recv()
        up_y[d] = push(up_at(block), up_at(block), y_peer)

    def forward_down(d):
        block = plane_at(-d) * 2 + side
        down_z[d].wait_recv()
        down_y[d] = push(down_at(block), down_at(block), y_peer)

    heads = q_all.shape[0]
    kv_heads = lanes // HD
    pairs_each = heads // 2 // kv_heads

    def attend(h):
        scores = lax.dot_general(
            q_all[h],
            kv_all[:, :lanes],
            (((1,), (1,)), ((), ())),
            preferred_element_type=jnp.float32,
        )
        exps = jnp.exp(scores - jnp.max(scores, axis=-1, keepdims=True))
        totals = jnp.sum(exps, axis=-1, keepdims=True)
        mixed = jnp.dot(
            exps.astype(jnp.bfloat16), kv_all[:, lanes:], preferred_element_type=jnp.float32
        )
        return mixed / totals

    def attend_pair(pair, carry):
        first, second = attend(2 * pair), attend(2 * pair + 1)
        low = pair < pairs_each
        left = jnp.where(low, first, pltpu.roll(first, HD, 1))
        right = jnp.where(low, pltpu.roll(second, HD, 1), second)
        lane = lax.broadcasted_iota(jnp.int32, left.shape, 1)
        head_all[pair] = jnp.where(lane < HD, left, right).astype(jnp.bfloat16)
        return carry

    lax.fori_loop(0, heads // 2, attend_pair, 0)
    forward_up(offsets[0])

    def columns(rank):
        return pl.ds(pl.multiple_of(rank * cols, cols), cols)

    def project(rank):
        total = jnp.zeros((rows, cols), jnp.float32)
        for pair in range(heads // 2):
            total += jnp.dot(
                head_all[pair],
                out_w_ref[pair * lanes : (pair + 1) * lanes, columns(rank)],
                preferred_element_type=jnp.float32,
            )
        return total.astype(jnp.bfloat16)

    far, near = (1 - ex) * 2, ex * 2
    first_send[0] = project(far + 1 - core)
    pass_far = push(first_send.at[0], first_land.at[0], core_peer)
    first_send[1] = project(near + 1 - core)
    pass_near = push(first_send.at[1], first_land.at[1], core_peer)
    far_own = project(far + core).astype(jnp.float32)
    pass_far.wait_recv()
    pair_send[...] = (far_own + first_land[0].astype(jnp.float32)).astype(jnp.bfloat16)
    pass_x = push(pair_send, pair_land, x_peer)
    near_own = project(near + core).astype(jnp.float32)
    pass_near.wait_recv()
    near_own += first_land[1].astype(jnp.float32)
    near_own += stream_ref[:, columns(own_tp)].astype(jnp.float32)
    pass_x.wait_recv()
    mid = (near_own + pair_land[...].astype(jnp.float32)).astype(jnp.bfloat16)
    mid_all[plane, own_tp] = mid

    own_mid = mid_all.at[plane, own_tp]
    mid_start, mid_arrive = line(lambda b: mid_all.at[b, own_tp], True)
    mid_start()
    mid_x = {0: push(own_mid, own_mid, x_peer)}
    mid_c = {0: push(own_mid, own_mid, core_peer)}
    mid_d = {}
    for d in offsets[1:]:
        forward_up(d)
    for d in offsets:
        forward_down(d)

    core_far, core_near, x_pass, z_pass = {}, {}, {}, {}

    def spread(d):
        mid_arrive(nearest(d))
        ref = mid_all.at[nearest(d), own_tp]
        mid_x[d] = push(ref, ref, x_peer)
        mid_c[d] = push(ref, ref, core_peer)

    z_base = take(planes)

    def z_copy(d, target, sender):
        return pltpu.make_async_remote_copy(
            src_ref=z_send.at[d],
            dst_ref=z_land.at[sender],
            send_sem=send_sems.at[z_base + d],
            recv_sem=recv_sems.at[z_base + sender],
            device_id=(target * 2 + side, own_tp),
            device_id_type=pl.DeviceIdType.MESH,
        )

    def mix(d):
        where_z = nearest(d)
        wide = [mid_all[where_z, r].astype(jnp.float32) for r in range(ranks)]
        square = sum(jnp.sum(w * w, axis=-1, keepdims=True) for w in wide)
        inverse = lax.rsqrt(square / (ranks * cols) + EPSILON)
        sums = jnp.zeros((rows, slab), jnp.float32)
        for r in range(ranks):
            normed = wide[r] * inverse * gain_ref[:, r * cols : (r + 1) * cols]
            sums += jnp.dot(
                normed.astype(jnp.bfloat16),
                up_all[r * cols : (r + 1) * cols, :],
                preferred_element_type=jnp.float32,
            )
        return jnp.square(jnp.maximum(sums, 0.0)).astype(jnp.bfloat16)

    def lower(hidden, rank):
        part = jnp.dot(hidden, down_all[:, columns(rank)], preferred_element_type=jnp.float32)
        return part.astype(jnp.bfloat16)

    def core_stage(d):
        hidden = mix(d)
        core_send[d, 0] = lower(hidden, far + 1 - core)
        core_far[d] = push(core_send.at[d, 0], core_land.at[d, 0], core_peer)
        core_send[d, 1] = lower(hidden, near + 1 - core)
        core_near[d] = push(core_send.at[d, 1], core_land.at[d, 1], core_peer)
        core_keep[d, 0] = lower(hidden, far + core)
        core_keep[d, 1] = lower(hidden, near + core)

    def x_stage(d):
        core_far[d].wait_recv()
        x_send[d] = (
            core_keep[d, 0].astype(jnp.float32) + core_land[d, 0].astype(jnp.float32)
        ).astype(jnp.bfloat16)
        x_pass[d] = push(x_send.at[d], x_land.at[d], x_peer)

    def z_stage(d):
        core_near[d].wait_recv()
        x_pass[d].wait_recv()
        total = core_keep[d, 1].astype(jnp.float32) + core_land[d, 1].astype(jnp.float32)
        total += x_land[d].astype(jnp.float32)
        z_send[d] = total.astype(jnp.bfloat16)
        if d:
            z_pass[d] = z_copy(d, nearest(d), plane)
            z_pass[d].start()
            copies.append(z_pass[d])

    for d in range(planes):
        if d + 1 < planes:
            spread(d + 1)
        mid_x[d].wait_recv()
        ref = mid_all.at[nearest(d), x_peer[1]]
        mid_d[d] = push(ref, ref, core_peer)
        if d == 0:
            for e in range(planes):
                up_y[e].wait_recv()
                down_y[e].wait_recv()
        mid_c[d].wait_recv()
        mid_d[d].wait_recv()
        core_stage(d)
        if d >= 1:
            x_stage(d - 1)
        if d >= 2:
            z_stage(d - 2)
    x_stage(planes - 1)
    for d in range(max(planes - 2, 0), planes):
        z_stage(d)
    total = mid_all[plane, own_tp].astype(jnp.float32) + z_send[0].astype(jnp.float32)
    for d in range(1, planes):
        sender = nearest(d)
        z_copy(d, sender, sender).wait_recv()
        total += z_land[sender].astype(jnp.float32)
    out_ref[...] = total.astype(jnp.bfloat16)
    for copy in copies:
        copy.wait_send()
    for valid, copy in guarded:
        pl.when(valid)(copy.wait_send)


def fused_shards(
    size_sp,
    size_tp,
    queries,
    keys,
    values,
    query_gain,
    key_gain,
    stream,
    out_weight,
    mixer_gain,
    up_weight,
    down_weight,
):
    planes = size_sp // 2
    rows, width = queries.shape
    lanes = keys.shape[1]
    heads = width // HD
    cols = stream.shape[1] // size_tp
    position = lax.axis_index("sp") * rows + jnp.arange(rows, dtype=jnp.int32)
    grid_row = (position // GRID_W).astype(jnp.float32)[:, None]
    grid_col = (position % GRID_W).astype(jnp.float32)[:, None]
    lane = jnp.arange(lanes, dtype=jnp.int32)
    pair = lane % HD // 2
    quarter = HD // 4
    inverse = 1.0 / jnp.power(10000.0, (pair % quarter * 2).astype(jnp.float32) / (HD // 2))
    angle = jnp.where(pair < quarter, grid_row, grid_col) * inverse
    sine = jnp.sin(angle)
    tables = jnp.stack([jnp.cos(angle), jnp.where(lane % 2 == 0, -sine, sine)])
    gains = jnp.stack([jnp.tile(query_gain, lanes // HD), jnp.tile(key_gain, lanes // HD)])
    slab = up_weight.shape[1] // planes
    half = jnp.bfloat16
    tile = (rows, cols)
    total_copies = 96
    vmem = pl.BlockSpec(memory_space=pltpu.VMEM)
    scratch = [
        pltpu.VMEM((heads, rows, lanes), half),
        pltpu.VMEM((size_sp * rows, 2 * lanes), half),
        pltpu.VMEM((stream.shape[1], slab), half),
        pltpu.VMEM((slab, stream.shape[1]), half),
        pltpu.VMEM((heads // 2, rows, lanes), half),
        pltpu.VMEM((2,) + tile, half),
        pltpu.VMEM((2,) + tile, half),
        pltpu.VMEM(tile, half),
        pltpu.VMEM(tile, half),
        pltpu.VMEM((planes, size_tp) + tile, half),
        pltpu.VMEM((planes, 2) + tile, half),
        pltpu.VMEM((planes, 2) + tile, half),
        pltpu.VMEM((planes, 2) + tile, half),
        pltpu.VMEM((planes,) + tile, half),
        pltpu.VMEM((planes,) + tile, half),
        pltpu.VMEM((planes,) + tile, half),
        pltpu.VMEM((planes,) + tile, half),
        pltpu.SemaphoreType.DMA((total_copies,)),
        pltpu.SemaphoreType.DMA((total_copies,)),
    ]
    return pl.pallas_call(
        functools.partial(layer_kernel, planes, size_tp),
        out_shape=jax.ShapeDtypeStruct(tile, half),
        in_specs=[vmem] * 10,
        out_specs=vmem,
        scratch_shapes=scratch,
        compiler_params=pltpu.CompilerParams(
            collective_id=0, has_side_effects=True, vmem_limit_bytes=60 * 2**20
        ),
        name="layer",
    )(queries, keys, values, tables, gains, stream, out_weight, mixer_gain[None, :], up_weight, down_weight)


def solution(mesh):
    size_sp, size_tp = mesh.shape["sp"], mesh.shape["tp"]

    def body(*arrays):
        tiled = arrays[9].shape[1] % 128 == 0 and arrays[1].shape[1] == 2 * HD
        if tiled and size_tp == 4 and size_sp % 2 == 0:
            return fused_shards(size_sp, size_tp, *arrays)
        return shards(*arrays)

    return jax.shard_map(
        body,
        mesh=mesh,
        in_specs=(
            P("sp", "tp"),
            P("sp", "tp"),
            P("sp", "tp"),
            P(),
            P(),
            P("sp", None),
            P("tp", None),
            P(),
            P("sp", "tp"),
            P("tp", "sp"),
        ),
        out_specs=P("sp", "tp"),
        check_vma=False,
    )
```
